512 devices in a mesh: kv: 64 (over z, y), tp: 8 (over x, core).
Axes of the slice: x: 4, y: 8, z: 8, core: 2. Of those that a mesh axis runs over, the one named last changes fastest.
Arguments:
- queries: bfloat16 [8192, 1024], P('kv', 'tp'), may hold values from -4 to 4
- keys: bfloat16 [8192, 1024], P('kv', 'tp'), may hold values from -4 to 4
- values: bfloat16 [8192, 1024], P('kv', 'tp'), may hold values from -4 to 4
- cotangent: bfloat16 [8192, 1024], P('kv', 'tp'), may hold values from -4 to 4
- log_sum: float32 [16, 8192], P('tp', 'kv'), may hold values from 4.5 to 7.5
- chosen: int32 [16, 256, 12], P('tp'), may hold values from 0 to 255, as said below
- normed_input: bfloat16 [8192, 2048], P('kv', 'tp'), may hold values from -0.0625 to 0.0625
Outputs:
- grad_queries: bfloat16 [8192, 1024], P('kv', 'tp')
- grad_keys: bfloat16 [8192, 1024], P('kv', 'tp')
- grad_values: bfloat16 [8192, 1024], P('kv', 'tp')
- grad_weight: float32 [2048, 1024], P('kv', 'tp')
The draws below stay inside these ranges and needn't reach their ends.
Inputs may be any that keep to these rules, and one draw needn't show every extreme that they name: `chosen`: for each head, the distinct blocks below their own query block that the query blocks of one device's 128 positions choose include at most 1 block of any one device's span of 128 positions, and exactly 1 for some pairs of devices. Within one list the entries below the query block's own index are distinct.
All inputs are finite; a program needn't handle non-finite values.
Results may differ from the reference program's by a relative error of at most 0.0085.
Values may be sent and summed in bfloat16 or wider, within the bound.
No kernel may reach another device: no remote copies, remote signals or barrier semaphores. Data moves between devices by JAX's collectives and lax.ppermute only.
A program may use at most 64 MiB of HBM per device.

```python
import jax
import jax.numpy as jnp
from jax import lax

D = 2048
HEADS = 16
HD = 64
BLK = 32
SEL = 12
MOST = 1
TOK_DEV = 128
TOKENS = 8192
WIDTH = 1024
N_KV = 64


def draw_chosen(key, part):
    devices = N_KV
    blocks_dev = TOK_DEV // BLK
    splits = jax.random.split(jax.random.fold_in(key, 17), 4)
    first_pick = jax.random.randint(splits[0], (HEADS, devices, devices), 0, blocks_dev)
    step_pick = jax.random.randint(splits[1], (HEADS, devices, devices), 1, blocks_dev)
    owner_ids = jnp.arange(devices, dtype=jnp.int32)
    cand_list = []
    for slot_index in range(MOST):
        local_pick = (first_pick + slot_index * step_pick) % blocks_dev
        cand_list.append(owner_ids[None, None, :] * blocks_dev + local_pick)
    candidates = jnp.stack(cand_list, axis=-1)
    popular = jax.random.randint(splits[2], (HEADS, 1, devices, 1), 0, 8)
    popular = popular * popular
    query_dev = owner_ids[None, :, None, None]
    owner_dev = owner_ids[None, None, :, None]
    boosted = jnp.where((owner_dev == query_dev - 1) | (owner_dev == query_dev - devices // 2), 2, 0)
    base_score = boosted * 64 + popular
    jitter = jax.random.randint(splits[3], (HEADS, devices, blocks_dev, devices, MOST), 0, 4096)
    query_ids = owner_ids[:, None] * blocks_dev + jnp.arange(blocks_dev, dtype=jnp.int32)[None, :]
    cand_rows = candidates[:, :, None, :, :]
    usable = cand_rows < query_ids[None, :, :, None, None]
    tie_break = jnp.arange(MOST * devices, dtype=jnp.int32).reshape(devices, MOST)
    scored = (base_score[:, :, None, :, :] * 4096 + jitter) * 256 + tie_break
    scored = jnp.where(usable, scored, -1).reshape(HEADS, devices, blocks_dev, MOST * devices)
    top_values, top_index = lax.top_k(scored, SEL)
    flat_cands = jnp.broadcast_to(cand_rows, (HEADS, devices, blocks_dev, devices, MOST)).reshape(HEADS, devices, blocks_dev, MOST * devices)
    picked = jnp.take_along_axis(flat_cands, top_index, axis=-1)
    picked = jnp.where(top_values >= 0, picked, query_ids[None, :, :, None])
    return picked.reshape(HEADS, devices * blocks_dev, SEL).astype(jnp.int32)


def block_levels(stream_key, shape, cuts, low, largest):
    level, own = 1.0, jax.random.fold_in(stream_key, 6)
    for dim, blocks in cuts:
        draws = jnp.exp(jax.random.uniform(jax.random.fold_in(own, dim), (blocks,), jnp.float32, low / len(cuts), largest / len(cuts)))
        level = level * jnp.repeat(draws, shape[dim] // blocks).reshape([-1 if axis == dim else 1 for axis in range(len(shape))])
    return level


def noise(own_key, shape, scale, most, pieces=(), kind=jnp.bfloat16):
    gain = block_levels(own_key, shape, pieces, -0.22, 0.18) if pieces else 1.0
    array = jax.random.normal(own_key, shape, jnp.float32) * scale * gain
    return jnp.minimum(jnp.maximum(array, -most), most).astype(kind)


def setup_inputs(seed: int = 0) -> dict:
    key_list = jax.random.split(jax.random.key(seed), 8)
    queries = noise(key_list[0], (TOKENS, WIDTH), 1.0, 4.0, ((0, 64), (1, 8)))
    keys = noise(key_list[1], (TOKENS, WIDTH), 1.0, 4.0, ((0, 64), (1, 8)))
    values = noise(key_list[2], (TOKENS, WIDTH), 1.0, 4.0, ((0, 64), (1, 8)))
    cotangent = noise(key_list[3], (TOKENS, WIDTH), 1.0, 4.0, ((0, 64), (1, 8)))
    log_sum = jnp.clip(4.5 + 3.0 * jax.random.uniform(key_list[4], (HEADS, TOKENS), jnp.float32) ** block_levels(key_list[4], (HEADS, TOKENS), ((0, 8), (1, 64)), -0.2, 0.2), 4.5, 7.5)
    chosen = draw_chosen(jax.random.fold_in(key_list[7], 71), 0)
    normed_input = noise(key_list[6], (TOKENS, D), TOKENS ** -0.5, 0.0625, ((0, 64), (1, 8)))
    return dict(queries=queries, keys=keys, values=values, cotangent=cotangent, log_sum=log_sum, chosen=chosen, normed_input=normed_input)


MASKED = -1e30


def reference(queries, keys, values, cotangent, log_sum, chosen, normed_input):
    token_count = queries.shape[0]
    block_total = token_count // BLK
    score_scale = HD ** -0.5
    block_ids = jnp.arange(block_total, dtype=jnp.int32)
    causal = jnp.arange(BLK)[:, None] >= jnp.arange(BLK)[None, :]

    def per_head(head_index):
        def columns(row_block):
            picked_cols = lax.dynamic_slice_in_dim(row_block, head_index * HD, HD, 1)
            return picked_cols.reshape(block_total, BLK, HD).astype(jnp.float32)

        q_blocks = columns(queries)
        k_blocks = columns(keys)
        v_blocks = columns(values)
        g_blocks = columns(cotangent)
        log_rows = lax.dynamic_index_in_dim(log_sum, head_index, 0, keepdims=False).reshape(block_total, BLK)[..., None]
        picked = lax.dynamic_index_in_dim(chosen, head_index, 0, keepdims=False).astype(jnp.int32)
        usable = picked < block_ids[:, None]
        safe_ids = jnp.where(usable, picked, 0).astype(jnp.int32)
        keys_all = jnp.concatenate([k_blocks[safe_ids].reshape(block_total, SEL * BLK, HD), k_blocks], axis=1)
        values_all = jnp.concatenate([v_blocks[safe_ids].reshape(block_total, SEL * BLK, HD), v_blocks], axis=1)
        sel_mask = jnp.broadcast_to(jnp.repeat(usable, BLK, axis=1)[:, None, :], (block_total, BLK, SEL * BLK))
        allowed = jnp.concatenate([sel_mask, jnp.broadcast_to(causal, (block_total, BLK, BLK))], axis=2)
        scores = jnp.einsum('jqd,jkd->jqk', q_blocks, keys_all) * score_scale
        weights = jnp.exp(jnp.where(allowed, scores - log_rows, MASKED))
        value_dots = jnp.einsum('jqd,jkd->jqk', g_blocks, values_all)
        row_delta = jnp.sum(weights * value_dots, axis=-1, keepdims=True)
        score_grad = lax.optimization_barrier((weights * (value_dots - row_delta)).astype(jnp.bfloat16)).astype(jnp.float32)
        weights_low = lax.optimization_barrier(weights.astype(jnp.bfloat16)).astype(jnp.float32)
        query_grad = jnp.einsum('jqk,jkd->jqd', score_grad, keys_all) * score_scale
        key_grad = jnp.einsum('jqk,jqd->jkd', score_grad, q_blocks) * score_scale
        value_grad = jnp.einsum('jqk,jqd->jkd', weights_low, g_blocks)

        def settle(gradient):
            spread = gradient[:, :SEL * BLK].reshape(block_total * SEL, BLK, HD)
            summed = jax.ops.segment_sum(spread, safe_ids.reshape(-1), num_segments=block_total)
            return (summed + gradient[:, SEL * BLK:]).reshape(token_count, HD).astype(jnp.bfloat16)

        return query_grad.reshape(token_count, HD).astype(jnp.bfloat16), settle(key_grad), settle(value_grad)

    head_grads = lax.map(per_head, jnp.arange(HEADS, dtype=jnp.int32))

    def joined_rows(stacked):
        return stacked.transpose(1, 0, 2).reshape(token_count, HEADS * HD)

    grad_queries = joined_rows(head_grads[0])
    grad_keys = joined_rows(head_grads[1])
    grad_values = joined_rows(head_grads[2])
    grad_weight = jnp.dot(normed_input.T, grad_queries, preferred_element_type=jnp.float32)
    return grad_queries, grad_keys, grad_values, grad_weight
```

```python
import jax
import jax.numpy as jnp
from jax import lax
from jax.experimental import pallas as pl
from jax.experimental.pallas import tpu as pltpu
from jax.sharding import PartitionSpec as P

HD = 64
BLK = 32
SEL = 12
MASKED = -1e30

F32 = jnp.float32
BF16 = jnp.bfloat16
VMEM = pl.BlockSpec(memory_space=pltpu.VMEM)
SMEM = pl.BlockSpec(memory_space=pltpu.SMEM)
NT = (((1,), (1,)), ((), ()))
NN = (((1,), (0,)), ((), ()))
TN = (((0,), (0,)), ((), ()))


def dot(a, b, dims):
    return lax.dot_general(a, b, dims, preferred_element_type=F32)


def pick_kernel(me_ref, chosen_ref, k_ref, v_ref, send_ref, ids_ref):
    heads, blocks, sel = chosen_ref.shape
    devices = send_ref.shape[0]
    blocks_dev = blocks // devices
    width = k_ref.shape[1]
    first = me_ref[0] * blocks_dev
    row = lax.broadcasted_iota(jnp.int32, (blocks, sel), 0)
    lane = lax.broadcasted_iota(jnp.int32, (blocks, width), 1)
    codes = jnp.zeros((blocks, width), F32)
    for h in range(heads):
        c = chosen_ref[h]
        d = c - first
        hit = (c < row) & (d >= 0) & (d < blocks_dev)
        code = jnp.where(hit, jnp.left_shift(1, 3 * jnp.where(hit, d, 0)), 0).astype(F32)
        codes = jnp.where(lane // HD == h, jnp.sum(code, axis=1, keepdims=True), codes)
    owner = lax.broadcasted_iota(jnp.int32, (devices, blocks), 0)
    block = lax.broadcasted_iota(jnp.int32, (devices, blocks), 1)
    group = jnp.where(block // blocks_dev == owner, 1.0, 0.0).astype(BF16)
    ids_ref[...] = dot(group, codes.astype(BF16), NN)
    kb = [k_ref[b * BLK : (b + 1) * BLK, :].astype(F32) for b in range(blocks_dev)]
    vb = [v_ref[b * BLK : (b + 1) * BLK, :].astype(F32) for b in range(blocks_dev)]

    def step(t, _):
        code = jnp.broadcast_to(ids_ref[pl.ds(t, 1), :], (BLK, width))
        ks, vs = kb[0], vb[0]
        for b in range(1, blocks_dev):
            m = code >= 8.0**b
            ks = jnp.where(m, kb[b], ks)
            vs = jnp.where(m, vb[b], vs)
        send_ref[t, 0:BLK, :] = ks.astype(BF16)
        send_ref[t, BLK : 2 * BLK, :] = vs.astype(BF16)
        return 0

    lax.fori_loop(0, devices, step, 0, unroll=4)


def grad_kernel(
    tiles_ref, q_ref, g_ref, k_ref, v_ref, bias_ref, lse_ref, xt_ref,
    send_ref, dq_ref, dk_ref, dv_ref, p_ref, d_ref,
):
    devices = tiles_ref.shape[0]
    rows, width = q_ref.shape
    heads = width // HD
    cols = heads * rows
    scale = HD**-0.5
    step_slots = 8
    chunk = step_slots * BLK
    lane = lax.broadcasted_iota(jnp.int32, (rows, width), 1)

    def by_head(x):
        return jnp.concatenate(
            [jnp.where(lane // HD == h, x, 0.0).astype(BF16) for h in range(heads)], axis=0
        )

    qm = by_head(q_ref[...].astype(F32))
    gm = by_head(g_ref[...].astype(F32))

    ko, vo = k_ref[...], v_ref[...]
    key_row = lax.broadcasted_iota(jnp.int32, (rows, cols), 0)
    query = lax.broadcasted_iota(jnp.int32, (rows, cols), 1) % rows
    own = (key_row // BLK == query // BLK) & (key_row <= query)
    p_own = jnp.exp(jnp.where(own, dot(ko, qm, NT) * scale - lse_ref[...], MASKED))
    d_own = dot(vo, gm, NT)
    delta0 = jnp.sum((p_own * d_own).reshape(rows // 8, 8, cols), axis=0)

    def forward(c, delta):
        keys = tiles_ref[pl.ds(c * step_slots, step_slots), 0:BLK, :].reshape(chunk, width)
        vals = tiles_ref[pl.ds(c * step_slots, step_slots), BLK : 2 * BLK, :].reshape(chunk, width)
        s = dot(keys, qm, NT) * scale
        d = dot(vals, gm, NT)
        for i in range(step_slots):
            b = bias_ref[pl.ds(c * step_slots + i, 1), :]
            sl = slice(i * BLK, (i + 1) * BLK)
            p = jnp.exp(s[sl] + b)
            at = pl.ds(pl.multiple_of(c * chunk + i * BLK, BLK), BLK)
            p_ref[at, :] = p
            d_ref[at, :] = d[sl]
            delta = delta + jnp.sum((p * d[sl]).reshape(BLK // 8, 8, cols), axis=0)
        return delta

    steps = devices // step_slots
    delta = lax.fori_loop(0, steps, forward, delta0, unroll=2)
    delta = jnp.sum(delta, axis=0, keepdims=True)

    ds_own = (p_own * (d_own - delta)).astype(BF16)
    dk_ref[...] = dot(ds_own, qm, NN) * scale
    dv_ref[...] = dot(p_own.astype(BF16), gm, NN)
    dqt0 = dot(ko, ds_own, TN)

    def backward(c, dqt):
        at = pl.ds(pl.multiple_of(c * chunk, chunk), chunk)
        p = p_ref[at, :]
        ds = (p * (d_ref[at, :] - delta)).astype(BF16)
        keys = tiles_ref[pl.ds(c * step_slots, step_slots), 0:BLK, :].reshape(chunk, width)
        dk = (dot(ds, qm, NN) * scale).astype(BF16)
        dv = dot(p.astype(BF16), gm, NN).astype(BF16)
        slots = pl.ds(c * step_slots, step_slots)
        send_ref[slots, 0:BLK, :] = dk.reshape(step_slots, BLK, width)
        send_ref[slots, BLK : 2 * BLK, :] = dv.reshape(step_slots, BLK, width)
        return dqt + dot(keys, ds, TN)

    dqt = lax.fori_loop(0, steps, backward, dqt0, unroll=2)
    head_of = lax.broadcasted_iota(jnp.int32, (width, rows), 0) // HD
    merged = dqt[:, 0:rows]
    for h in range(1, heads):
        merged = jnp.where(head_of == h, dqt[:, h * rows : (h + 1) * rows], merged)
    dq = (jnp.transpose(merged) * scale).astype(BF16)
    dq_ref[...] = dq
    piece = xt_ref.shape[0] // devices
    w = dot(xt_ref[...], dq, NN).astype(BF16)
    send_ref[:, 2 * BLK : 2 * BLK + piece, :] = w.reshape(devices, piece, width)


def settle_kernel(back_ref, ids_ref, dk_ref, dv_ref, gk_ref, gv_ref, gw_ref):
    devices = back_ref.shape[0]
    rows, width = dk_ref.shape
    blocks_dev = rows // BLK
    piece = gw_ref.shape[0]
    start = tuple(dk_ref[b * BLK : (b + 1) * BLK, :] for b in range(blocks_dev))
    start += tuple(dv_ref[b * BLK : (b + 1) * BLK, :] for b in range(blocks_dev))
    start += (jnp.zeros((piece, width), F32),)

    def step(t, sums):
        code = jnp.broadcast_to(ids_ref[pl.ds(t, 1), :], (BLK, width))
        dk = back_ref[t, 0:BLK, :].astype(F32)
        dv = back_ref[t, BLK : 2 * BLK, :].astype(F32)
        w = back_ref[t, 2 * BLK : 2 * BLK + piece, :].astype(F32)
        out_k, out_v = [], []
        for b in range(blocks_dev):
            m = (code >= 8.0**b) & (code < 8.0 ** (b + 1))
            out_k.append(sums[b] + jnp.where(m, dk, 0.0))
            out_v.append(sums[blocks_dev + b] + jnp.where(m, dv, 0.0))
        return tuple(out_k) + tuple(out_v) + (sums[-1] + w,)

    sums = lax.fori_loop(0, devices, step, start, unroll=2)
    for b in range(blocks_dev):
        gk_ref[b * BLK : (b + 1) * BLK, :] = sums[b].astype(BF16)
        gv_ref[b * BLK : (b + 1) * BLK, :] = sums[blocks_dev + b].astype(BF16)
    gw_ref[...] = sums[-1]


def body(queries, keys, values, cotangent, log_sum, chosen, normed_input):
    rows, width = queries.shape
    heads, block_total, _ = chosen.shape
    blocks_dev = rows // BLK
    devices = lax.axis_size("kv")
    me = lax.axis_index("kv")
    shape = jax.ShapeDtypeStruct

    send, ids = pl.pallas_call(
        pick_kernel,
        out_shape=(shape((devices, 2 * BLK, width), BF16), shape((devices, width), F32)),
        in_specs=[SMEM, VMEM, VMEM, VMEM],
        out_specs=(VMEM, VMEM),
        name="pick",
    )(me.astype(jnp.int32).reshape(1), chosen, keys, values)
    tiles = lax.all_to_all(send, "kv", split_axis=0, concat_axis=0, tiled=True)

    xt = lax.all_gather(normed_input.T, "tp", axis=0, tiled=True)
    own_ids = me * blocks_dev + jnp.arange(blocks_dev, dtype=jnp.int32)
    lists = lax.dynamic_slice_in_dim(chosen, me * blocks_dev, blocks_dev, 1)
    owners = jnp.where(lists < own_ids[None, :, None], lists // blocks_dev, -1)
    slots = jnp.arange(devices, dtype=jnp.int32)
    asked = jnp.any(owners[None] == slots[:, None, None, None], axis=-1)
    bias = jnp.where(
        asked[..., None], -log_sum.reshape(1, heads, blocks_dev, BLK), MASKED
    ).reshape(devices, heads * rows)
    lse = log_sum.reshape(1, heads * rows)

    piece = xt.shape[0] // devices
    send2, dq, dk, dv = pl.pallas_call(
        grad_kernel,
        out_shape=(
            shape((devices, 2 * BLK + piece, width), BF16),
            shape((rows, width), BF16),
            shape((rows, width), F32),
            shape((rows, width), F32),
        ),
        in_specs=[VMEM] * 8,
        out_specs=(VMEM,) * 4,
        scratch_shapes=[
            pltpu.VMEM((devices * BLK, heads * rows), F32),
            pltpu.VMEM((devices * BLK, heads * rows), F32),
        ],
        name="grads",
    )(tiles, queries, cotangent, keys, values, bias, lse, xt)
    back = lax.all_to_all(send2, "kv", split_axis=0, concat_axis=0, tiled=True)
    gk, gv, gw = pl.pallas_call(
        settle_kernel,
        out_shape=(
            shape((rows, width), BF16),
            shape((rows, width), BF16),
            shape((piece, width), F32),
        ),
        in_specs=[VMEM] * 4,
        out_specs=(VMEM,) * 3,
        name="settle",
    )(back, ids, dk, dv)
    return (dq, gk, gv, gw)


def solution(mesh):
    in_specs = (
        P("kv", "tp"),
        P("kv", "tp"),
        P("kv", "tp"),
        P("kv", "tp"),
        P("tp", "kv"),
        P("tp", None, None),
        P("kv", "tp"),
    )
    out_specs = (P("kv", "tp"), P("kv", "tp"), P("kv", "tp"), P("kv", "tp"))
    return jax.shard_map(body, mesh=mesh, in_specs=in_specs, out_specs=out_specs, check_vma=False)
```

```python
import jax
import jax.numpy as jnp
from jax import lax
from jax.experimental import pallas as pl
from jax.experimental.pallas import tpu as pltpu
from jax.sharding import PartitionSpec as P

HD = 64
BLK = 32
SEL = 12
MASKED = -1e30

F32 = jnp.float32
BF16 = jnp.bfloat16
VMEM = pl.BlockSpec(memory_space=pltpu.VMEM)
SMEM = pl.BlockSpec(memory_space=pltpu.SMEM)
NT = (((1,), (1,)), ((), ()))
NN = (((1,), (0,)), ((), ()))
TN = (((0,), (0,)), ((), ()))


def dot(a, b, dims):
    return lax.dot_general(a, b, dims, preferred_element_type=F32)


def pick_kernel(me_ref, chosen_ref, k_ref, v_ref, send_ref, ids_ref):
    sel, heads, blocks = chosen_ref.shape
    devices = send_ref.shape[0]
    blocks_dev = blocks // devices
    width = k_ref.shape[1]
    first = me_ref[0] * blocks_dev
    d = chosen_ref[...] - first
    asking = lax.broadcasted_iota(jnp.int32, (sel, heads, blocks), 2) - first
    hit = (d < asking) & (d >= 0) & (d < blocks_dev)
    code = jnp.zeros(d.shape, F32)
    for b in range(blocks_dev):
        code = jnp.where(hit & (d == b), 8.0**b, code)
    code = jnp.sum(code, axis=0)
    row = lax.broadcasted_iota(jnp.int32, (width, blocks), 0)
    codes = jnp.broadcast_to(code[0:1, :], (width, blocks))
    for h in range(1, heads):
        codes = jnp.where(row // HD == h, code[h : h + 1, :], codes)
    owner = lax.broadcasted_iota(jnp.int32, (devices, blocks), 0)
    block = lax.broadcasted_iota(jnp.int32, (devices, blocks), 1)
    group = jnp.where(block // blocks_dev == owner, 1.0, 0.0).astype(BF16)
    ids_ref[...] = dot(group, codes.astype(BF16), NT)
    kb = [k_ref[b * BLK : (b + 1) * BLK, :].astype(F32) for b in range(blocks_dev)]
    vb = [v_ref[b * BLK : (b + 1) * BLK, :].astype(F32) for b in range(blocks_dev)]

    def step(t, _):
        code = jnp.broadcast_to(ids_ref[pl.ds(t, 1), :], (BLK, width))
        ks, vs = kb[0], vb[0]
        for b in range(1, blocks_dev):
            m = code >= 8.0**b
            ks = jnp.where(m, kb[b], ks)
            vs = jnp.where(m, vb[b], vs)
        send_ref[t, 0:BLK, :] = ks.astype(BF16)
        send_ref[t, BLK : 2 * BLK, :] = vs.astype(BF16)
        return 0

    lax.fori_loop(0, devices, step, 0, unroll=4)


def grad_kernel(
    tiles_ref, q_ref, g_ref, k_ref, v_ref, bias_ref, lse_ref, xt_ref,
    send_ref, dq_ref, dk_ref, dv_ref, p_ref, d_ref,
):
    devices = tiles_ref.shape[0]
    rows, width = q_ref.shape
    heads = width // HD
    cols = heads * rows
    scale = HD**-0.5
    step_slots = 8
    chunk = step_slots * BLK
    lane = lax.broadcasted_iota(jnp.int32, (rows, width), 1)

    def by_head(x):
        return jnp.concatenate(
            [jnp.where(lane // HD == h, x, 0.0).astype(BF16) for h in range(heads)], axis=0
        )

    qm = by_head(q_ref[...].astype(F32))
    gm = by_head(g_ref[...].astype(F32))

    ko, vo = (k_ref[...].astype(F32) * scale).astype(BF16), v_ref[...]
    key_row = lax.broadcasted_iota(jnp.int32, (rows, cols), 0)
    query = lax.broadcasted_iota(jnp.int32, (rows, cols), 1) % rows
    own = (key_row // BLK == query // BLK) & (key_row <= query)
    p_own = jnp.exp(jnp.where(own, dot(ko, qm, NT) - lse_ref[...], MASKED))
    d_own = dot(vo, gm, NT)
    delta0 = jnp.sum((p_own * d_own).reshape(rows // 8, 8, cols), axis=0)

    def forward(c, delta):
        keys = tiles_ref[pl.ds(c * step_slots, step_slots), 0:BLK, :].reshape(chunk, width)
        vals = tiles_ref[pl.ds(c * step_slots, step_slots), BLK : 2 * BLK, :].reshape(chunk, width)
        s = dot(keys, qm, NT)
        d = dot(vals, gm, NT)
        for i in range(step_slots):
            b = bias_ref[pl.ds(c * step_slots + i, 1), :]
            sl = slice(i * BLK, (i + 1) * BLK)
            p = jnp.exp(s[sl] + b)
            at = pl.ds(pl.multiple_of(c * chunk + i * BLK, BLK), BLK)
            p_ref[at, :] = p
            d_ref[at, :] = d[sl]
            delta = delta + jnp.sum((p * d[sl]).reshape(BLK // 8, 8, cols), axis=0)
        return delta

    steps = devices // step_slots
    delta = lax.fori_loop(0, steps, forward, delta0, unroll=2)
    delta = jnp.sum(delta, axis=0, keepdims=True)

    ds_own = (p_own * (d_own - delta)).astype(BF16)
    dk_ref[...] = dot(ds_own, qm, NN) * scale
    dv_ref[...] = dot(p_own.astype(BF16), gm, NN)
    dqt0 = dot(ko, ds_own, TN)

    def backward(c, dqt):
        at = pl.ds(pl.multiple_of(c * chunk, chunk), chunk)
        p = p_ref[at, :]
        ds = (p * (d_ref[at, :] - delta)).astype(BF16)
        keys = tiles_ref[pl.ds(c * step_slots, step_slots), 0:BLK, :].reshape(chunk, width)
        dk = (dot(ds, qm, NN) * scale).astype(BF16)
        dv = dot(p.astype(BF16), gm, NN).astype(BF16)
        slots = pl.ds(c * step_slots, step_slots)
        send_ref[slots, 0:BLK, :] = dk.reshape(step_slots, BLK, width)
        send_ref[slots, BLK : 2 * BLK, :] = dv.reshape(step_slots, BLK, width)
        return dqt + dot(keys, ds, TN)

    dqt = lax.fori_loop(0, steps, backward, dqt0, unroll=2)
    head_of = lax.broadcasted_iota(jnp.int32, (width, rows), 0) // HD
    merged = dqt[:, 0:rows]
    for h in range(1, heads):
        merged = jnp.where(head_of == h, dqt[:, h * rows : (h + 1) * rows], merged)
    dq = jnp.transpose(merged).astype(BF16)
    dq_ref[...] = dq
    piece = xt_ref.shape[0] // devices
    w = dot(xt_ref[...], dq, NN).astype(BF16)
    send_ref[:, 2 * BLK : 2 * BLK + piece, :] = w.reshape(devices, piece, width)


def settle_kernel(back_ref, ids_ref, dk_ref, dv_ref, gk_ref, gv_ref, gw_ref):
    devices = back_ref.shape[0]
    rows, width = dk_ref.shape
    blocks_dev = rows // BLK
    piece = gw_ref.shape[0]
    start = tuple(dk_ref[b * BLK : (b + 1) * BLK, :] for b in range(blocks_dev))
    start += tuple(dv_ref[b * BLK : (b + 1) * BLK, :] for b in range(blocks_dev))
    start += (jnp.zeros((piece, width), F32),)

    def step(t, sums):
        code = ids_ref[pl.ds(t, 1), :]
        dk = back_ref[t, 0:BLK, :].astype(F32)
        dv = back_ref[t, BLK : 2 * BLK, :].astype(F32)
        w = back_ref[t, 2 * BLK : 2 * BLK + piece, :].astype(F32)
        out_k, out_v = [], []
        for b in range(blocks_dev):
            m = jnp.where((code >= 8.0**b) & (code < 8.0 ** (b + 1)), 1.0, 0.0)
            out_k.append(sums[b] + m * dk)
            out_v.append(sums[blocks_dev + b] + m * dv)
        return tuple(out_k) + tuple(out_v) + (sums[-1] + w,)

    sums = lax.fori_loop(0, devices, step, start, unroll=2)
    for b in range(blocks_dev):
        gk_ref[b * BLK : (b + 1) * BLK, :] = sums[b].astype(BF16)
        gv_ref[b * BLK : (b + 1) * BLK, :] = sums[blocks_dev + b].astype(BF16)
    gw_ref[...] = sums[-1]


def body(queries, keys, values, cotangent, log_sum, chosen, normed_input):
    rows, width = queries.shape
    heads, block_total, _ = chosen.shape
    blocks_dev = rows // BLK
    devices = lax.axis_size("kv")
    me = lax.axis_index("kv")
    shape = jax.ShapeDtypeStruct

    def near(x):
        return pltpu.with_memory_space_constraint(x, pltpu.VMEM)

    send, ids = pl.pallas_call(
        pick_kernel,
        out_shape=(pltpu.VMEM((devices, 2 * BLK, width), BF16), pltpu.VMEM((devices, width), F32)),
        in_specs=[SMEM, VMEM, VMEM, VMEM],
        out_specs=(VMEM, VMEM),
        name="pick",
    )(me.astype(jnp.int32).reshape(1), near(chosen.transpose(2, 0, 1)), near(keys), near(values))
    tiles = lax.all_to_all(send, "kv", split_axis=0, concat_axis=0, tiled=True)

    key_rows = jnp.arange(2 * BLK) < BLK
    tiles = tiles * jnp.where(key_rows, HD**-0.5, 1.0).astype(BF16)[None, :, None]

    xt = lax.all_gather(normed_input.T, "tp", axis=0, tiled=True)
    own_ids = me * blocks_dev + jnp.arange(blocks_dev, dtype=jnp.int32)
    lists = lax.dynamic_slice_in_dim(chosen, me * blocks_dev, blocks_dev, 1)
    owners = jnp.where(lists < own_ids[None, :, None], lists // blocks_dev, -1)
    slots = jnp.arange(devices, dtype=jnp.int32)
    asked = jnp.any(owners[None] == slots[:, None, None, None], axis=-1)
    bias = jnp.where(
        asked[..., None], -log_sum.reshape(1, heads, blocks_dev, BLK), MASKED
    ).reshape(devices, heads * rows)
    lse = log_sum.reshape(1, heads * rows)

    piece = xt.shape[0] // devices
    send2, dq, dk, dv = pl.pallas_call(
        grad_kernel,
        out_shape=(
            pltpu.VMEM((devices, 2 * BLK + piece, width), BF16),
            shape((rows, width), BF16),
            pltpu.VMEM((rows, width), F32),
            pltpu.VMEM((rows, width), F32),
        ),
        in_specs=[VMEM] * 8,
        out_specs=(VMEM,) * 4,
        scratch_shapes=[
            pltpu.VMEM((devices * BLK, heads * rows), F32),
            pltpu.VMEM((devices * BLK, heads * rows), F32),
        ],
        name="grads",
    )(*map(near, (tiles, queries, cotangent, keys, values, bias, lse, xt)))
    back = lax.all_to_all(send2, "kv", split_axis=0, concat_axis=0, tiled=True)
    gk, gv, gw = pl.pallas_call(
        settle_kernel,
        out_shape=(
            shape((rows, width), BF16),
            shape((rows, width), BF16),
            shape((piece, width), F32),
        ),
        in_specs=[VMEM] * 4,
        out_specs=(VMEM,) * 3,
        name="settle",
    )(*map(near, (back, ids, dk, dv)))
    return (dq, gk, gv, gw)


def solution(mesh):
    in_specs = (
        P("kv", "tp"),
        P("kv", "tp"),
        P("kv", "tp"),
        P("kv", "tp"),
        P("tp", "kv"),
        P("tp", None, None),
        P("kv", "tp"),
    )
    out_specs = (P("kv", "tp"), P("kv", "tp"), P("kv", "tp"), P("kv", "tp"))
    return jax.shard_map(body, mesh=mesh, in_specs=in_specs, out_specs=out_specs, check_vma=False)
```
